32 devices in a mesh: sp: 8 (over z, y), tp: 4 (over x, core).
Axes of the slice: x: 2, y: 2, z: 4, core: 2. Of those that a mesh axis runs over, the one named last changes fastest.
Arguments:
- memory_queries: bfloat16 [4096, 1024], P('sp', 'tp'), may hold values from -8 to 8
- memory_keys: bfloat16 [4096, 1024], P('sp', 'tp'), may hold values from -8 to 8
- memory_values: bfloat16 [4096, 1024], P('sp', 'tp'), may hold values from -6 to 6
- input_gate_logits: float32 [8, 4096], P('tp', 'sp'), may hold values from -64 to 160
- forget_gate_logits: float32 [8, 4096], P('tp', 'sp'), may hold values from -0.1 to 20
- extra_log_decay: float32 [8, 4096], P('tp', 'sp'), may hold values from -1.4 to 0
- residual: bfloat16 [4096, 2048], P(('sp', 'tp')), may hold values from -6 to 6
- cell_output_weight: bfloat16 [1024, 2048], P('tp', 'sp'), may hold values from -0.1875 to 0.1875
- expert_norm_gain: float32 [2048], replicated, may hold values from 0.1 to 1.9
- expert_gate_weight: bfloat16 [8, 2048, 3584], P('sp', None, 'tp'), may hold values from -0.125 to 0.125
- expert_up_weight: bfloat16 [8, 2048, 3584], P('sp', None, 'tp'), may hold values from -0.125 to 0.125
- expert_down_weight: bfloat16 [8, 3584, 2048], P('sp', 'tp'), may hold values from -0.09375 to 0.09375
- routed_expert_index: int32 [4096, 2], P('sp'), may hold values from 0 to 7, as said below
- routed_expert_weight: float32 [4096, 2], P(('sp', 'tp')), may hold values from 0.1 to 1
Outputs:
- layer_out: bfloat16 [4096, 2048], P(('sp', 'tp'))
The draws below stay inside these ranges and needn't reach their ends.
Inputs may be any that keep to these rules, and one draw needn't show every extreme that they name: `routed_expert_index`: each row names 2 different experts. In each aligned block of 128 rows (the rows of one device after the cell) no expert is named more than 40 times, and one expert is named exactly 40 times in every block.
All inputs are finite; a program needn't handle non-finite values.
Results may differ from the reference program's by a relative error of at most 0.013.
Values may be sent and summed in bfloat16 or wider, within the bound.
A program may use at most 128 MiB of HBM per device.

```python
import math
import jax
import jax.numpy as jnp
from jax import lax

D = 2048
RECURRENT_LANES = 8
DH = 128
FF = 3584
TOPK = 2
TOK_DEV = 512
TEXT_LENGTH = 4096
ROWS = 128
HD = 1024
EXPERTS = 8
CAP = 40
EXPERT_ROWS = 1280
N_TP = 4


def shared_direction(key):
    return jnp.clip(jax.random.normal(jax.random.fold_in(key, 3), (RECURRENT_LANES * DH,), jnp.float32), -4.0, 4.0)


def query_like(key, salt_id):
    offset = 0.95
    dims_all = (TEXT_LENGTH, RECURRENT_LANES * DH)
    jitter = jnp.clip(jax.random.normal(jax.random.fold_in(key, salt_id), dims_all, jnp.float32), -4.0, 4.0)
    return jitter + offset * shared_direction(key)[None, :]


def draw_memory_queries(key, part):
    return query_like(key, 5).astype(jnp.bfloat16)


def draw_memory_keys(key, part):
    return query_like(key, 6).astype(jnp.bfloat16)


def draw_input_gate_logits(key, part):
    dims_all = (RECURRENT_LANES, TEXT_LENGTH)
    return 2.5 * jnp.clip(jax.random.normal(jax.random.fold_in(key, 8), dims_all, jnp.float32), -4.0, 4.0)


def draw_forget_gate_logits(key, part):
    ranking = jax.random.permutation(jax.random.fold_in(key, 12), RECURRENT_LANES)
    quick_count = RECURRENT_LANES // 2
    center = jnp.where(ranking < quick_count, math.log(40.0), math.log(TEXT_LENGTH) + 1.5).astype(jnp.float32)
    device_shift = jax.random.uniform(jax.random.fold_in(key, 13), (TEXT_LENGTH // TOK_DEV,), jnp.float32, -0.7, 0.7)
    device_shift = jnp.repeat(device_shift, TOK_DEV)
    jitter = jnp.clip(jax.random.normal(jax.random.fold_in(key, 14), (RECURRENT_LANES, TEXT_LENGTH), jnp.float32), -3.0, 3.0)
    return center[:, None] + device_shift[None, :] + jitter


def draw_extra_log_decay(key, part):
    surge_offset = jax.random.randint(jax.random.fold_in(key, 15), (RECURRENT_LANES, 3, 1), 0, TEXT_LENGTH)
    element_levels = jax.random.uniform(jax.random.fold_in(key, 16), (RECURRENT_LANES, 3, 1), jnp.float32, -0.69, -0.22)
    seat_locations = jnp.arange(TEXT_LENGTH)[None, None, :]
    return jnp.sum(jnp.where(seat_locations == surge_offset, element_levels, 0.0), axis=1)


def draw_routed_expert_index(key, part):
    specialist_capacity = EXPERTS * CAP
    assigned = ROWS * TOPK
    specialist_table = jnp.arange(specialist_capacity) // CAP
    favour_increment = jax.random.randint(jax.random.fold_in(key, 21), (EXPERTS,), 0, 3) * 4096
    chosen_specialists = jax.random.randint(jax.random.fold_in(key, 22), (), 0, EXPERTS)
    additional_reward = favour_increment[specialist_table] + jnp.where(specialist_table == chosen_specialists, 16384, 0)

    def one_block(address_tile_range):
        dispatch_affinity = jax.random.randint(jax.random.fold_in(address_tile_range, 1), (specialist_capacity,), 0, 4096) + additional_reward
        ranked = dispatch_affinity * specialist_capacity + jnp.arange(specialist_capacity)
        picked = lax.top_k(ranked, assigned)[1]
        names = jnp.sort(specialist_table[picked]).reshape(TOPK, ROWS).T
        turn = jax.random.randint(jax.random.fold_in(address_tile_range, 2), (ROWS, 1), 0, TOPK)
        names = jnp.take_along_axis(names, (jnp.arange(TOPK)[None, :] + turn) % TOPK, axis=1)
        return names[jax.random.permutation(jax.random.fold_in(address_tile_range, 3), ROWS)]
    block_keys = jax.random.split(jax.random.fold_in(key, 23), TEXT_LENGTH // ROWS)
    return jax.vmap(one_block)(block_keys).reshape(TEXT_LENGTH, TOPK).astype(jnp.int32)


def level_of(own_key, shape, cuts, smallest, largest):
    level = 1.0
    for axis_at, shards_of in cuts:
        draws = jax.random.uniform(jax.random.fold_in(jax.random.fold_in(own_key, 6), axis_at), (shards_of,), jnp.float32, smallest / len(cuts), largest / len(cuts))
        level = level * jnp.repeat(jnp.exp(draws), shape[axis_at] // shards_of).reshape((-1,) + (1,) * (len(shape) - 1 - axis_at))
    return level


def gaussian(rng, dims, scale, bound, shards=(), held_as=jnp.bfloat16):
    drawn = jax.random.normal(rng, dims, jnp.float32) * scale
    if len(shards) > 0:
        drawn = level_of(rng, dims, shards, -0.22, 0.18) * drawn
    return jnp.clip(drawn, min=-bound, max=bound).astype(held_as)


def setup_inputs(seed: int = 0) -> dict:
    key_list = jax.random.split(jax.random.key(seed), 15)
    return {
        "memory_queries": draw_memory_queries(jax.random.fold_in(key_list[14], 71), 0),
        "memory_keys": draw_memory_keys(jax.random.fold_in(key_list[14], 71), 0),
        "memory_values": gaussian(key_list[2], (TEXT_LENGTH, HD), 1.0, 6.0, ((0, 8), (1, 4))),
        "input_gate_logits": draw_input_gate_logits(jax.random.fold_in(key_list[14], 71), 0),
        "forget_gate_logits": draw_forget_gate_logits(jax.random.fold_in(key_list[14], 71), 0),
        "extra_log_decay": draw_extra_log_decay(jax.random.fold_in(key_list[14], 71), 0),
        "residual": gaussian(key_list[6], (TEXT_LENGTH, D), 1.0, 6.0, ((0, 32),)),
        "cell_output_weight": gaussian(key_list[7], (HD, D), HD ** -0.5, 0.1875, ((0, 4), (1, 8))),
        "expert_norm_gain": jnp.clip(1.0 + 0.18 * jax.random.normal(key_list[8], (D,), jnp.float32), 0.1, 1.9),
        "expert_gate_weight": gaussian(key_list[9], (EXPERTS, D, FF), D ** -0.5, 0.125, ((0, 8), (2, 4))),
        "expert_up_weight": gaussian(key_list[10], (EXPERTS, D, FF), D ** -0.5, 0.125, ((0, 8), (2, 4))),
        "expert_down_weight": gaussian(key_list[11], (EXPERTS, FF, D), FF ** -0.5, 0.09375, ((0, 8), (1, 4))),
        "routed_expert_index": draw_routed_expert_index(jax.random.fold_in(key_list[14], 71), 0),
        "routed_expert_weight": jnp.clip(0.1 + 0.9 * jax.random.uniform(key_list[13], (TEXT_LENGTH, TOPK), jnp.float32) ** level_of(key_list[13], (TEXT_LENGTH, TOPK), ((0, 32),), -0.2, 0.2), 0.1, 1.0),
    }


highest = lax.Precision.HIGHEST
lowest = -1e+30
epsilon = 1e-06

def block_pass(memory, inputs):
    state_mat, state_norm, state_max = memory
    queries, keys_blk, values_blk, gate_in, forget_log_value = inputs
    length = gate_in.shape[-1]
    running = jnp.cumsum(forget_log_value, axis=-1)
    causal = jnp.arange(length)[:, None] >= jnp.arange(length)[None, :]
    exponent = running[:, :, None] - running[:, None, :] + gate_in[:, None, :]
    exponent = jnp.where(causal[None], exponent, -jnp.inf)
    carried = running + state_max[:, None]
    row_max = jnp.maximum(carried, lax.optimization_barrier(jnp.max(exponent, axis=-1)))
    decays = jnp.exp(exponent - row_max[:, :, None])
    carry_scale = jnp.exp(carried - row_max)
    dispatch_affinity = jnp.einsum('htk,hsk->hts', queries, keys_blk, precision=highest) * decays
    numerator = carry_scale[:, :, None] * jnp.einsum('hvk,htk->htv', state_mat, queries, precision=highest)
    numerator = numerator + jnp.einsum('hts,hsv->htv', dispatch_affinity, values_blk, precision=highest)
    denominator = carry_scale * jnp.einsum('hk,htk->ht', state_norm, queries, precision=highest) + lax.optimization_barrier(jnp.sum(dispatch_affinity, axis=-1))
    final_log = running[:, -1]
    log_prev = final_log + state_max
    log_keep = final_log[:, None] - running + gate_in
    new_max = jnp.maximum(log_prev, lax.optimization_barrier(jnp.max(log_keep, axis=-1)))
    prev_scale = jnp.exp(log_prev - new_max)
    retain = jnp.exp(log_keep - new_max[:, None])
    new_mat = prev_scale[:, None, None] * state_mat + jnp.einsum('hsv,hsk->hvk', retain[:, :, None] * values_blk, keys_blk, precision=highest)
    new_norm = prev_scale[:, None] * state_norm + jnp.einsum('hs,hsk->hk', retain, keys_blk, precision=highest)
    output = numerator / jnp.maximum(jnp.abs(denominator), jnp.exp(-row_max))[:, :, None]
    return ((new_mat, new_norm, new_max), output)

def heads_first(tensor):
    return jnp.transpose(tensor.astype(jnp.float32).reshape(TEXT_LENGTH, RECURRENT_LANES, DH), (1, 0, 2))

def reference(memory_queries, memory_keys, memory_values, input_gate_logits, forget_gate_logits, extra_log_decay, residual, cell_output_weight, expert_norm_gain, expert_gate_weight, expert_up_weight, expert_down_weight, routed_expert_index, routed_expert_weight):
    block_size = min(TOK_DEV, 256)
    block_count = TEXT_LENGTH // block_size

    def split_blocks(tensor):
        return jnp.moveaxis(tensor.reshape((RECURRENT_LANES, block_count, block_size) + tensor.shape[2:]), 1, 0)
    queries = heads_first(memory_queries) * DH ** (-0.5)
    forget_log_value = jax.nn.log_sigmoid(forget_gate_logits) + extra_log_decay
    start_state = (jnp.zeros((RECURRENT_LANES, DH, DH), jnp.float32), jnp.zeros((RECURRENT_LANES, DH), jnp.float32), jnp.full((RECURRENT_LANES,), lowest, jnp.float32))
    members = (queries, heads_first(memory_keys), heads_first(memory_values), input_gate_logits, forget_log_value)
    end_state, outputs = lax.scan(block_pass, start_state, tuple((split_blocks(member) for member in members)))
    hidden = jnp.moveaxis(outputs, 0, 1).reshape(RECURRENT_LANES, TEXT_LENGTH, DH).astype(jnp.bfloat16)
    flat_hidden = jnp.transpose(hidden, (1, 0, 2)).reshape(TEXT_LENGTH, HD)
    quarter = HD // N_TP
    projected = jnp.zeros((TEXT_LENGTH, D), jnp.float32)
    for owner_idx in range(N_TP):
        low_col = owner_idx * quarter
        group_term = jnp.dot(flat_hidden[:, low_col:low_col + quarter], cell_output_weight[low_col:low_col + quarter], preferred_element_type=jnp.float32)
        projected = projected + lax.optimization_barrier(group_term.astype(jnp.bfloat16)).astype(jnp.float32)
    mixed_rows = (residual.astype(jnp.float32) + projected).astype(jnp.bfloat16)
    mixed_wide = mixed_rows.astype(jnp.float32)
    norm_scale = lax.rsqrt(lax.optimization_barrier(jnp.mean(mixed_wide * mixed_wide, axis=-1, keepdims=True)) + epsilon)
    normed = (mixed_wide * norm_scale * expert_norm_gain).astype(jnp.bfloat16)
    normed_pad = jnp.concatenate([normed, jnp.zeros((1, D), jnp.bfloat16)], axis=0)
    hidden_part = FF // N_TP

    def one_expert(running_sum, expert):
        matched = routed_expert_index == expert
        weight_tok = jnp.concatenate([lax.optimization_barrier(jnp.sum(jnp.where(matched, routed_expert_weight, 0.0), axis=1)), jnp.zeros((1,), jnp.float32)])
        picked = jnp.nonzero(jnp.any(matched, axis=1), size=EXPERT_ROWS, fill_value=TEXT_LENGTH)[0]
        rows_in = normed_pad[picked]
        gate_all = expert_gate_weight[expert]
        up_all = expert_up_weight[expert]
        down_all = expert_down_weight[expert]
        result = jnp.zeros((EXPERT_ROWS, D), jnp.float32)
        for owner_idx in range(N_TP):
            low_col = owner_idx * hidden_part
            gate_pre = jnp.dot(rows_in, gate_all[:, low_col:low_col + hidden_part], preferred_element_type=jnp.float32)
            up_pre = jnp.dot(rows_in, up_all[:, low_col:low_col + hidden_part], preferred_element_type=jnp.float32)
            hidden_act = (jax.nn.silu(gate_pre) * up_pre).astype(jnp.bfloat16)
            group_term = jnp.dot(hidden_act, down_all[low_col:low_col + hidden_part], preferred_element_type=jnp.float32)
            result = result + lax.optimization_barrier(group_term.astype(jnp.bfloat16)).astype(jnp.float32)
        returned = lax.optimization_barrier(result.astype(jnp.bfloat16)).astype(jnp.float32)
        return (running_sum.at[picked].add(returned * weight_tok[picked][:, None], mode='drop'), None)
    routed, _ = lax.scan(one_expert, jnp.zeros((TEXT_LENGTH, D), jnp.float32), jnp.arange(EXPERTS, dtype=jnp.int32))
    return (mixed_wide + routed).astype(jnp.bfloat16)
```

```python
import functools
import jax
import jax.numpy as jnp
from jax import lax
from jax.experimental import pallas as pl
from jax.experimental.pallas import tpu as pltpu
from jax.sharding import PartitionSpec as P

highest = lax.Precision.HIGHEST
lowest = -1e30
epsilon = 1e-06


def places():
    sp, tp = lax.axis_index("sp"), lax.axis_index("tp")
    n = lax.axis_size("sp")
    return sp, tp, n, tp + 1 - 2 * (tp % 2), (tp + 2) % 4


def greet(devices):
    barrier = pltpu.get_barrier_semaphore()
    for device in devices:
        pl.semaphore_signal(
            barrier, inc=1, device_id=device, device_id_type=pl.DeviceIdType.MESH
        )
    pl.semaphore_wait(barrier, len(devices))


def remote(src, dst, send, recv, device):
    return pltpu.make_async_remote_copy(
        src_ref=src,
        dst_ref=dst,
        send_sem=send,
        recv_sem=recv,
        device_id=device,
        device_id_type=pl.DeviceIdType.MESH,
    )


def dispatch_kernel(x_ref, out_ref, send_sems, recv_sems):
    sp, tp, n, p, q = places()
    peers = [((sp + k) % n, tp) for k in range(1, n)]
    greet(peers + [(sp, p), (sp, q)])
    started, across = [], []
    first = [None]
    for k in range(1, n):
        copy = remote(
            x_ref.at[(sp + k) % n], out_ref.at[tp, sp],
            send_sems.at[0, k], recv_sems.at[0, k], peers[k - 1],
        )
        copy.start()
        first.append(copy)
    started += first[1:]
    late = []

    def relay(k):
        across[k].wait_recv()
        s = (sp - k + n) % n
        copy = remote(
            out_ref.at[q, s], out_ref.at[q, s], send_sems.at[3, k], recv_sems.at[3, k], (sp, p)
        )
        copy.start()
        late.append(copy)

    for k in range(n):
        s = (sp - k + n) % n
        if k == 0:
            src = x_ref.at[sp]
        else:
            first[k].wait_recv()
            src = out_ref.at[tp, s]
        copy = remote(src, out_ref.at[tp, s], send_sems.at[1, k], recv_sems.at[1, k], (sp, q))
        copy.start()
        across.append(copy)
        copy = remote(src, out_ref.at[tp, s], send_sems.at[2, k], recv_sems.at[2, k], (sp, p))
        copy.start()
        late.append(copy)
        if k == 0:
            out_ref[tp, sp] = x_ref[sp]
        else:
            relay(k - 1)
    relay(n - 1)
    for copy in late:
        copy.wait()
    for copy in started + across:
        copy.wait_send()


def dispatch(x):
    n, rows, width = x.shape
    return pl.pallas_call(
        dispatch_kernel,
        out_shape=jax.ShapeDtypeStruct((4, n, rows, width), x.dtype),
        in_specs=[pl.BlockSpec(memory_space=pltpu.VMEM)],
        out_specs=pl.BlockSpec(memory_space=pltpu.VMEM),
        scratch_shapes=[pltpu.SemaphoreType.DMA((4, n)), pltpu.SemaphoreType.DMA((4, n))],
        compiler_params=pltpu.CompilerParams(
            collective_id=1, has_side_effects=True, vmem_limit_bytes=58 * 2**20
        ),
    )(x)


def collect_kernel(back, x_ref, out_ref, near, sent, far, result, send_sems, recv_sems):
    sp, tp, n, p, q = places()
    chunks = x_ref.shape[1]
    peers = [((sp + k) % n, tp) for k in range(1, n)] if back else []
    greet(peers + [(sp, p), (sp, q)])

    def at(k):
        return (sp + 1 + k) % n if back else k

    near_far, near_own, crossing, homeward = [], [], [], []
    for k in range(chunks):
        copy = remote(
            x_ref.at[(p + 2) % 4, at(k)], near.at[0, k],
            send_sems.at[0, k], recv_sems.at[0, k], (sp, p),
        )
        copy.start()
        near_far.append(copy)
    for k in range(chunks):
        copy = remote(
            x_ref.at[p, at(k)], near.at[1, k], send_sems.at[1, k], recv_sems.at[1, k], (sp, p)
        )
        copy.start()
        near_own.append(copy)
    for k in range(chunks):
        near_far[k].wait_recv()
        total = x_ref[q, at(k)].astype(jnp.float32) + near[0, k].astype(jnp.float32)
        sent[k] = total.astype(jnp.bfloat16)
        copy = remote(sent.at[k], far.at[k], send_sems.at[2, k], recv_sems.at[2, k], (sp, q))
        copy.start()
        crossing.append(copy)
    for k in range(chunks):
        near_own[k].wait_recv()
        crossing[k].wait_recv()
        total = x_ref[tp, at(k)].astype(jnp.float32) + near[1, k].astype(jnp.float32)
        total = (total + far[k].astype(jnp.float32)).astype(jnp.bfloat16)
        if not back:
            out_ref[k] = total
        elif k == chunks - 1:
            out_ref[sp] = total
        else:
            result[k] = total
            copy = remote(
                result.at[k], out_ref.at[sp], send_sems.at[3, k], recv_sems.at[3, k], peers[k]
            )
            copy.start()
            homeward.append(copy)
    for copy in homeward:
        copy.wait()
    for copy in near_far + near_own + crossing:
        copy.wait_send()


def collect(x, back):
    _, n, rows, width = x.shape
    block = (n, rows, width)
    return pl.pallas_call(
        functools.partial(collect_kernel, back),
        out_shape=jax.ShapeDtypeStruct(block, x.dtype),
        in_specs=[pl.BlockSpec(memory_space=pltpu.VMEM)],
        out_specs=pl.BlockSpec(memory_space=pltpu.VMEM),
        scratch_shapes=[
            pltpu.VMEM((2,) + block, x.dtype),
            pltpu.VMEM(block, x.dtype),
            pltpu.VMEM(block, x.dtype),
            pltpu.VMEM(block if back else (1, 16, 128), x.dtype),
            pltpu.SemaphoreType.DMA((4, n)),
            pltpu.SemaphoreType.DMA((4, n)),
        ],
        compiler_params=pltpu.CompilerParams(
            collective_id=2 if back else 3, has_side_effects=True, vmem_limit_bytes=58 * 2**20
        ),
    )(x)


def spread_kernel(x_ref, out_ref, send_sems, recv_sems):
    sp, tp, n, _, _ = places()
    half = n // 2
    twin = sp + 1 - 2 * (sp % 2)
    peers = [((sp + 2 * k) % n, tp) for k in range(1, half)]
    greet(peers + [(twin, tp)])
    first, second = [None], []
    for k in range(1, half):
        copy = remote(
            x_ref, out_ref.at[sp], send_sems.at[0, k], recv_sems.at[0, k], peers[k - 1]
        )
        copy.start()
        first.append(copy)
    for k in range(half):
        s = (sp - 2 * k + n) % n
        if k == 0:
            src = x_ref
        else:
            first[k].wait_recv()
            src = out_ref.at[s]
        copy = remote(src, out_ref.at[s], send_sems.at[1, k], recv_sems.at[1, k], (twin, tp))
        copy.start()
        second.append(copy)
        if k == 0:
            out_ref[sp] = x_ref[...]
    for copy in second:
        copy.wait()
    for copy in first[1:]:
        copy.wait_send()


def spread(x):
    n = lax.axis_size("sp")
    half = n // 2
    return pl.pallas_call(
        spread_kernel,
        out_shape=jax.ShapeDtypeStruct((n,) + x.shape, x.dtype),
        in_specs=[pl.BlockSpec(memory_space=pltpu.VMEM)],
        out_specs=pl.BlockSpec(memory_space=pltpu.VMEM),
        scratch_shapes=[pltpu.SemaphoreType.DMA((2, half)), pltpu.SemaphoreType.DMA((2, half))],
        compiler_params=pltpu.CompilerParams(
            collective_id=4, has_side_effects=True, vmem_limit_bytes=58 * 2**20
        ),
    )(x)


def carried_in(x):
    log_sum, mat, norm, top = x
    heads, dim, _ = mat.shape
    n, place = lax.axis_size("sp"), lax.axis_index("sp")
    scalars = jnp.broadcast_to(jnp.concatenate([log_sum, top])[:, None], (2 * heads, dim))
    packed = jnp.concatenate([mat.reshape(heads * dim, dim), norm, scalars], axis=0)
    used = packed.shape[0]
    packed = jnp.pad(packed, ((0, -used % 8), (0, 0)))
    everything = spread(packed)
    mats = everything[:, : heads * dim].reshape(n, heads, dim, dim)
    norms = everything[:, heads * dim : heads * dim + heads]
    logs = everything[:, heads * dim + heads : heads * dim + 2 * heads, 0]
    tops = everything[:, heads * dim + 2 * heads : heads * dim + 3 * heads, 0]
    index = jnp.arange(n)
    reached = index < place
    between = (index[None, :] > index[:, None]) & reached[None, :]
    decay = jnp.sum(jnp.where(between[:, :, None], logs[None], 0.0), axis=1)
    level = jnp.where(reached[:, None], tops + decay, lowest)
    prior_max = jnp.max(level, axis=0)
    scale = jnp.where(reached[:, None], jnp.exp(level - prior_max), 0.0)
    prior_mat = jnp.sum(scale[:, :, None, None] * mats, axis=0)
    prior_norm = jnp.sum(scale[:, :, None] * norms, axis=0)
    return prior_mat, prior_norm, prior_max


def block_pass(memory, inputs):
    state_mat, state_norm, state_max = memory
    queries, keys_blk, values_blk, gate_in, forget_log_value = inputs
    length = gate_in.shape[-1]
    running = jnp.cumsum(forget_log_value, axis=-1)
    causal = jnp.arange(length)[:, None] >= jnp.arange(length)[None, :]
    exponent = running[:, :, None] - running[:, None, :] + gate_in[:, None, :]
    exponent = jnp.where(causal[None], exponent, -jnp.inf)
    carried = running + state_max[:, None]
    row_max = jnp.maximum(carried, jnp.max(exponent, axis=-1))
    decays = jnp.exp(exponent - row_max[:, :, None])
    carry_scale = jnp.exp(carried - row_max)
    dispatch_affinity = jnp.einsum("htk,hsk->hts", queries, keys_blk, precision=highest) * decays
    numerator = carry_scale[:, :, None] * jnp.einsum(
        "hvk,htk->htv", state_mat, queries, precision=highest
    )
    numerator = numerator + jnp.einsum(
        "hts,hsv->htv", dispatch_affinity, values_blk, precision=highest
    )
    denominator = carry_scale * jnp.einsum(
        "hk,htk->ht", state_norm, queries, precision=highest
    ) + jnp.sum(dispatch_affinity, axis=-1)
    final_log = running[:, -1]
    log_prev = final_log + state_max
    log_keep = final_log[:, None] - running + gate_in
    new_max = jnp.maximum(log_prev, jnp.max(log_keep, axis=-1))
    prev_scale = jnp.exp(log_prev - new_max)
    retain = jnp.exp(log_keep - new_max[:, None])
    new_mat = prev_scale[:, None, None] * state_mat + jnp.einsum(
        "hsv,hsk->hvk", retain[:, :, None] * values_blk, keys_blk, precision=highest
    )
    new_norm = prev_scale[:, None] * state_norm + jnp.einsum(
        "hs,hsk->hk", retain, keys_blk, precision=highest
    )
    return ((new_mat, new_norm, new_max), (numerator, denominator, row_max))


def matrix_memory_step(
    memory_queries,
    memory_keys,
    memory_values,
    input_gate_logits,
    forget_gate_logits,
    extra_log_decay,
):
    tokens_here, channels = memory_queries.shape
    heads_here = input_gate_logits.shape[0]
    head_dim = channels // heads_here

    def heads_first(tensor):
        return jnp.transpose(
            tensor.astype(jnp.float32).reshape(tokens_here, heads_here, head_dim), (1, 0, 2)
        )

    queries = heads_first(memory_queries) * head_dim ** (-0.5)
    forget_log_value = jax.nn.log_sigmoid(forget_gate_logits) + extra_log_decay
    block_size = min(tokens_here, 256)
    block_count = tokens_here // block_size

    def split_blocks(tensor):
        return jnp.moveaxis(
            tensor.reshape((heads_here, block_count, block_size) + tensor.shape[2:]), 1, 0
        )

    def join_blocks(tensor):
        return jnp.moveaxis(tensor, 0, 1).reshape((heads_here, tokens_here) + tensor.shape[3:])

    empty_state = (
        jnp.zeros((heads_here, head_dim, head_dim), jnp.float32),
        jnp.zeros((heads_here, head_dim), jnp.float32),
        jnp.full((heads_here,), lowest, jnp.float32),
    )
    members = (
        queries,
        heads_first(memory_keys),
        heads_first(memory_values),
        input_gate_logits,
        forget_log_value,
    )
    end_state, pieces = lax.scan(
        block_pass, empty_state, tuple((split_blocks(member) for member in members))
    )
    numerator, denominator, row_max = (join_blocks(member) for member in pieces)
    running = jnp.cumsum(forget_log_value, axis=-1)
    prior_mat, prior_norm, prior_max = carried_in((running[:, -1],) + tuple(end_state))
    reached = running + prior_max[:, None]
    joined = jnp.maximum(row_max, reached)
    local_scale = jnp.exp(row_max - joined)
    carry_scale = jnp.exp(reached - joined)
    numerator = local_scale[:, :, None] * numerator + carry_scale[:, :, None] * jnp.einsum(
        "hvk,htk->htv", prior_mat, queries, precision=highest
    )
    denominator = local_scale * denominator + carry_scale * jnp.einsum(
        "hk,htk->ht", prior_norm, queries, precision=highest
    )
    guarded = jnp.maximum(jnp.abs(denominator), jnp.exp(-joined))
    return ((numerator / guarded[:, :, None]).astype(jnp.bfloat16), heads_here, head_dim)


def slot_index(ids, experts, capacity):
    flat_ids = ids.reshape(-1)
    matches = (flat_ids[:, None] == jnp.arange(experts, dtype=jnp.int32)[None, :]).astype(jnp.int32)
    before = jnp.cumsum(matches, axis=0) - matches
    return flat_ids * capacity + jnp.sum(before * matches, axis=1)


def local(
    memory_queries,
    memory_keys,
    memory_values,
    input_gate_logits,
    forget_gate_logits,
    extra_log_decay,
    residual,
    cell_output_weight,
    expert_norm_gain,
    expert_gate_weight,
    expert_up_weight,
    expert_down_weight,
    routed_expert_index,
    routed_expert_weight,
):
    hidden, heads_here, head_dim = matrix_memory_step(
        memory_queries,
        memory_keys,
        memory_values,
        input_gate_logits,
        forget_gate_logits,
        extra_log_decay,
    )
    weight_piece = lax.all_gather(cell_output_weight, "sp", axis=1, tiled=True)
    shaped = weight_piece.reshape(heads_here, head_dim, weight_piece.shape[1])
    partial_rows = jnp.einsum(
        "htd,hdc->tc", hidden, shaped, preferred_element_type=jnp.float32
    ).astype(jnp.bfloat16)
    row_count, model_width = residual.shape
    projected = collect(partial_rows.reshape(4, 4, row_count // 4, model_width), False)
    projected = projected.reshape(row_count, model_width).astype(jnp.float32)
    mixed_rows = (residual.astype(jnp.float32) + projected).astype(jnp.bfloat16)
    mixed_wide = mixed_rows.astype(jnp.float32)
    norm_scale = lax.rsqrt(jnp.mean(mixed_wide * mixed_wide, axis=-1, keepdims=True) + epsilon)
    normed = (mixed_wide * norm_scale * expert_norm_gain).astype(jnp.bfloat16)
    sp_size = lax.axis_size("sp")
    top_count = routed_expert_index.shape[1]
    experts = sp_size * expert_gate_weight.shape[0]
    assigned = row_count * top_count
    capacity = max(2, assigned * 5 // (4 * experts))
    own_ids = lax.dynamic_slice_in_dim(
        routed_expert_index, lax.axis_index("tp") * row_count, row_count, 0
    )
    own_slots = slot_index(own_ids, experts, capacity)
    zero_row = jnp.zeros((1, model_width), jnp.bfloat16)
    padded = jnp.concatenate([normed, zero_row], axis=0)
    slot_table = jnp.full((experts * capacity,), row_count, jnp.int32)
    slot_table = slot_table.at[own_slots].set(jnp.arange(assigned, dtype=jnp.int32) // top_count)
    arrived = dispatch(padded[slot_table.reshape(experts, capacity)])
    flat_rows = arrived.reshape(-1, model_width)
    gate_pre = jnp.dot(flat_rows, expert_gate_weight[0], preferred_element_type=jnp.float32)
    up_pre = jnp.dot(flat_rows, expert_up_weight[0], preferred_element_type=jnp.float32)
    hidden_act = (jax.nn.silu(gate_pre) * up_pre).astype(jnp.bfloat16)
    group_term = jnp.dot(hidden_act, expert_down_weight[0], preferred_element_type=jnp.float32)
    group_term = lax.optimization_barrier(group_term.astype(jnp.bfloat16)).astype(jnp.float32)
    returned = collect(group_term.astype(jnp.bfloat16).reshape(arrived.shape), True)
    picked = returned.reshape(experts * capacity, model_width)[own_slots]
    picked = picked.reshape(row_count, top_count, model_width).astype(jnp.float32)
    routed_sum = jnp.sum(picked * routed_expert_weight[:, :, None], axis=1)
    return (mixed_wide + routed_sum).astype(jnp.bfloat16)


def solution(mesh):
    return jax.shard_map(
        local,
        mesh=mesh,
        in_specs=(
            P("sp", "tp"),
            P("sp", "tp"),
            P("sp", "tp"),
            P("tp", "sp"),
            P("tp", "sp"),
            P("tp", "sp"),
            P(("sp", "tp"), None),
            P("tp", "sp"),
            P(),
            P("sp", None, "tp"),
            P("sp", None, "tp"),
            P("sp", "tp", None),
            P("sp", None),
            P(("sp", "tp"), None),
        ),
        out_specs=P(("sp", "tp"), None),
        check_vma=False,
    )
```

```python
import functools
import jax
import jax.numpy as jnp
from jax import lax
from jax.experimental import pallas as pl
from jax.experimental.pallas import tpu as pltpu
from jax.sharding import PartitionSpec as P

highest = lax.Precision.HIGHEST
lowest = -1e30
epsilon = 1e-06


def places():
    sp, tp = lax.axis_index("sp"), lax.axis_index("tp")
    n = lax.axis_size("sp")
    return sp, tp, n, tp + 1 - 2 * (tp % 2), (tp + 2) % 4


def greet(devices):
    barrier = pltpu.get_barrier_semaphore()
    for device in devices:
        pl.semaphore_signal(
            barrier, inc=1, device_id=device, device_id_type=pl.DeviceIdType.MESH
        )
    pl.semaphore_wait(barrier, len(devices))


def remote(src, dst, send, recv, device):
    return pltpu.make_async_remote_copy(
        src_ref=src,
        dst_ref=dst,
        send_sem=send,
        recv_sem=recv,
        device_id=device,
        device_id_type=pl.DeviceIdType.MESH,
    )


def far_first(n):
    return sorted(range(1, n), key=lambda k: abs(2 * k - n))


def dispatch_kernel(x_ref, out_ref, send_sems, recv_sems):
    sp, tp, n, p, q = places()
    peers = [((sp + k) % n, tp) for k in range(1, n)]
    greet(peers + [(sp, p), (sp, q)])
    across, first, late = {}, {}, []
    for k in far_first(n):
        copy = remote(
            x_ref.at[(sp + k) % n], out_ref.at[tp, sp],
            send_sems.at[0, k], recv_sems.at[0, k], peers[k - 1],
        )
        copy.start()
        first[k] = copy

    def relay(k):
        across[k].wait_recv()
        s = (sp - k + n) % n
        copy = remote(
            out_ref.at[q, s], out_ref.at[q, s], send_sems.at[3, k], recv_sems.at[3, k], (sp, p)
        )
        copy.start()
        late.append(copy)

    order = [0] + far_first(n)
    for step, k in enumerate(order):
        s = (sp - k + n) % n
        if k == 0:
            src = x_ref.at[sp]
        else:
            first[k].wait_recv()
            src = out_ref.at[tp, s]
        copy = remote(src, out_ref.at[tp, s], send_sems.at[1, k], recv_sems.at[1, k], (sp, q))
        copy.start()
        across[k] = copy
        copy = remote(src, out_ref.at[tp, s], send_sems.at[2, k], recv_sems.at[2, k], (sp, p))
        copy.start()
        late.append(copy)
        if k == 0:
            out_ref[tp, sp] = x_ref[sp]
        else:
            relay(order[step - 1])
    relay(order[-1])
    for copy in late:
        copy.wait()
    for copy in list(first.values()) + list(across.values()):
        copy.wait_send()


def dispatch(x):
    n, rows, width = x.shape
    return pl.pallas_call(
        dispatch_kernel,
        out_shape=jax.ShapeDtypeStruct((4, n, rows, width), x.dtype),
        in_specs=[pl.BlockSpec(memory_space=pltpu.VMEM)],
        out_specs=pl.BlockSpec(memory_space=pltpu.VMEM),
        scratch_shapes=[pltpu.SemaphoreType.DMA((4, n)), pltpu.SemaphoreType.DMA((4, n))],
        compiler_params=pltpu.CompilerParams(
            collective_id=1, has_side_effects=True, vmem_limit_bytes=58 * 2**20
        ),
    )(x)


def collect_kernel(back, x_ref, out_ref, near, sent, far, result, send_sems, recv_sems):
    sp, tp, n, p, q = places()
    chunks = x_ref.shape[1]
    offsets = far_first(n) + [0]
    peers = [((sp + k) % n, tp) for k in offsets[:-1]] if back else []
    greet(peers + [(sp, p), (sp, q)])

    def at(k):
        return (sp + offsets[k]) % n if back else k

    near_far, near_own, crossing, homeward = [], [], [], []
    for k in range(chunks):
        copy = remote(
            x_ref.at[(p + 2) % 4, at(k)], near.at[0, k],
            send_sems.at[0, k], recv_sems.at[0, k], (sp, p),
        )
        copy.start()
        near_far.append(copy)
    for k in range(chunks):
        copy = remote(
            x_ref.at[p, at(k)], near.at[1, k], send_sems.at[1, k], recv_sems.at[1, k], (sp, p)
        )
        copy.start()
        near_own.append(copy)
    for k in range(chunks):
        near_far[k].wait_recv()
        total = x_ref[q, at(k)].astype(jnp.float32) + near[0, k].astype(jnp.float32)
        sent[k] = total.astype(jnp.bfloat16)
        copy = remote(sent.at[k], far.at[k], send_sems.at[2, k], recv_sems.at[2, k], (sp, q))
        copy.start()
        crossing.append(copy)
    for k in range(chunks):
        near_own[k].wait_recv()
        crossing[k].wait_recv()
        total = x_ref[tp, at(k)].astype(jnp.float32) + near[1, k].astype(jnp.float32)
        total = (total + far[k].astype(jnp.float32)).astype(jnp.bfloat16)
        if not back:
            out_ref[k] = total
        elif k == chunks - 1:
            out_ref[sp] = total
        else:
            result[k] = total
            copy = remote(
                result.at[k], out_ref.at[sp], send_sems.at[3, k], recv_sems.at[3, k], peers[k]
            )
            copy.start()
            homeward.append(copy)
    for copy in homeward:
        copy.wait()
    for copy in near_far + near_own + crossing:
        copy.wait_send()


def collect(x, back):
    _, n, rows, width = x.shape
    block = (n, rows, width)
    return pl.pallas_call(
        functools.partial(collect_kernel, back),
        out_shape=jax.ShapeDtypeStruct(block, x.dtype),
        in_specs=[pl.BlockSpec(memory_space=pltpu.VMEM)],
        out_specs=pl.BlockSpec(memory_space=pltpu.VMEM),
        scratch_shapes=[
            pltpu.VMEM((2,) + block, x.dtype),
            pltpu.VMEM(block, x.dtype),
            pltpu.VMEM(block, x.dtype),
            pltpu.VMEM(block if back else (1, 16, 128), x.dtype),
            pltpu.SemaphoreType.DMA((4, n)),
            pltpu.SemaphoreType.DMA((4, n)),
        ],
        compiler_params=pltpu.CompilerParams(
            collective_id=2 if back else 3, has_side_effects=True, vmem_limit_bytes=58 * 2**20
        ),
    )(x)


def spread_kernel(x_ref, out_ref, send_sems, recv_sems):
    sp, tp, n, _, _ = places()
    half = n // 2
    twin = sp + 1 - 2 * (sp % 2)
    peers = [((sp + 2 * k) % n, tp) for k in range(1, half)]
    greet(peers + [(twin, tp)])
    first, second = [None], []
    for k in range(1, half):
        copy = remote(
            x_ref, out_ref.at[sp], send_sems.at[0, k], recv_sems.at[0, k], peers[k - 1]
        )
        copy.start()
        first.append(copy)
    for k in range(half):
        s = (sp - 2 * k + n) % n
        if k == 0:
            src = x_ref
        else:
            first[k].wait_recv()
            src = out_ref.at[s]
        copy = remote(src, out_ref.at[s], send_sems.at[1, k], recv_sems.at[1, k], (twin, tp))
        copy.start()
        second.append(copy)
        if k == 0:
            out_ref[sp] = x_ref[...]
    for copy in second:
        copy.wait()
    for copy in first[1:]:
        copy.wait_send()


def spread(x):
    n = lax.axis_size("sp")
    half = n // 2
    return pl.pallas_call(
        spread_kernel,
        out_shape=jax.ShapeDtypeStruct((n,) + x.shape, x.dtype),
        in_specs=[pl.BlockSpec(memory_space=pltpu.VMEM)],
        out_specs=pl.BlockSpec(memory_space=pltpu.VMEM),
        scratch_shapes=[pltpu.SemaphoreType.DMA((2, half)), pltpu.SemaphoreType.DMA((2, half))],
        compiler_params=pltpu.CompilerParams(
            collective_id=4, has_side_effects=True, vmem_limit_bytes=58 * 2**20
        ),
    )(x)


def carried_in(x):
    log_sum, mat, norm, top = x
    heads, dim, _ = mat.shape
    n, place = lax.axis_size("sp"), lax.axis_index("sp")
    scalars = jnp.broadcast_to(jnp.concatenate([log_sum, top])[:, None], (2 * heads, dim))
    packed = jnp.concatenate([mat.reshape(heads * dim, dim), norm, scalars], axis=0)
    used = packed.shape[0]
    packed = jnp.pad(packed, ((0, -used % 8), (0, 0)))
    everything = spread(packed)
    mats = everything[:, : heads * dim].reshape(n, heads, dim, dim)
    norms = everything[:, heads * dim : heads * dim + heads]
    logs = everything[:, heads * dim + heads : heads * dim + 2 * heads, 0]
    tops = everything[:, heads * dim + 2 * heads : heads * dim + 3 * heads, 0]
    index = jnp.arange(n)
    reached = index < place
    between = (index[None, :] > index[:, None]) & reached[None, :]
    decay = jnp.sum(jnp.where(between[:, :, None], logs[None], 0.0), axis=1)
    level = jnp.where(reached[:, None], tops + decay, lowest)
    prior_max = jnp.max(level, axis=0)
    scale = jnp.where(reached[:, None], jnp.exp(level - prior_max), 0.0)
    prior_mat = jnp.sum(scale[:, :, None, None] * mats, axis=0)
    prior_norm = jnp.sum(scale[:, :, None] * norms, axis=0)
    return prior_mat, prior_norm, prior_max


def block_pass(memory, inputs):
    state_mat, state_norm, state_max = memory
    queries, keys_blk, values_blk, gate_in, forget_log_value = inputs
    length = gate_in.shape[-1]
    running = jnp.cumsum(forget_log_value, axis=-1)
    causal = jnp.arange(length)[:, None] >= jnp.arange(length)[None, :]
    exponent = running[:, :, None] - running[:, None, :] + gate_in[:, None, :]
    exponent = jnp.where(causal[None], exponent, -jnp.inf)
    carried = running + state_max[:, None]
    row_max = jnp.maximum(carried, jnp.max(exponent, axis=-1))
    decays = jnp.exp(exponent - row_max[:, :, None])
    carry_scale = jnp.exp(carried - row_max)
    dispatch_affinity = jnp.einsum("htk,hsk->hts", queries, keys_blk, precision=highest) * decays
    numerator = carry_scale[:, :, None] * jnp.einsum(
        "hvk,htk->htv", state_mat, queries, precision=highest
    )
    numerator = numerator + jnp.einsum(
        "hts,hsv->htv", dispatch_affinity, values_blk, precision=highest
    )
    denominator = carry_scale * jnp.einsum(
        "hk,htk->ht", state_norm, queries, precision=highest
    ) + jnp.sum(dispatch_affinity, axis=-1)
    final_log = running[:, -1]
    log_prev = final_log + state_max
    log_keep = final_log[:, None] - running + gate_in
    new_max = jnp.maximum(log_prev, jnp.max(log_keep, axis=-1))
    prev_scale = jnp.exp(log_prev - new_max)
    retain = jnp.exp(log_keep - new_max[:, None])
    new_mat = prev_scale[:, None, None] * state_mat + jnp.einsum(
        "hsv,hsk->hvk", retain[:, :, None] * values_blk, keys_blk, precision=highest
    )
    new_norm = prev_scale[:, None] * state_norm + jnp.einsum(
        "hs,hsk->hk", retain, keys_blk, precision=highest
    )
    return ((new_mat, new_norm, new_max), (numerator, denominator, row_max))


def matrix_memory_step(
    memory_queries,
    memory_keys,
    memory_values,
    input_gate_logits,
    forget_gate_logits,
    extra_log_decay,
):
    tokens_here, channels = memory_queries.shape
    heads_here = input_gate_logits.shape[0]
    head_dim = channels // heads_here

    def heads_first(tensor):
        pieces = [
            tensor[:, head * head_dim : (head + 1) * head_dim] for head in range(heads_here)
        ]
        return jnp.stack(pieces).astype(jnp.float32)

    queries = heads_first(memory_queries) * head_dim ** (-0.5)
    forget_log_value = jax.nn.log_sigmoid(forget_gate_logits) + extra_log_decay
    block_size = min(tokens_here, 256)
    block_count = tokens_here // block_size

    def split_blocks(tensor):
        return jnp.moveaxis(
            tensor.reshape((heads_here, block_count, block_size) + tensor.shape[2:]), 1, 0
        )

    def join_blocks(tensor):
        return jnp.moveaxis(tensor, 0, 1).reshape((heads_here, tokens_here) + tensor.shape[3:])

    empty_state = (
        jnp.zeros((heads_here, head_dim, head_dim), jnp.float32),
        jnp.zeros((heads_here, head_dim), jnp.float32),
        jnp.full((heads_here,), lowest, jnp.float32),
    )
    members = (
        queries,
        heads_first(memory_keys),
        heads_first(memory_values),
        input_gate_logits,
        forget_log_value,
    )
    end_state, pieces = lax.scan(
        block_pass, empty_state, tuple((split_blocks(member) for member in members))
    )
    numerator, denominator, row_max = (join_blocks(member) for member in pieces)
    running = jnp.cumsum(forget_log_value, axis=-1)
    prior_mat, prior_norm, prior_max = carried_in((running[:, -1],) + tuple(end_state))
    reached = running + prior_max[:, None]
    joined = jnp.maximum(row_max, reached)
    local_scale = jnp.exp(row_max - joined)
    carry_scale = jnp.exp(reached - joined)
    numerator = local_scale[:, :, None] * numerator + carry_scale[:, :, None] * jnp.einsum(
        "hvk,htk->htv", prior_mat, queries, precision=highest
    )
    denominator = local_scale * denominator + carry_scale * jnp.einsum(
        "hk,htk->ht", prior_norm, queries, precision=highest
    )
    guarded = jnp.maximum(jnp.abs(denominator), jnp.exp(-joined))
    return ((numerator / guarded[:, :, None]).astype(jnp.bfloat16), heads_here, head_dim)


def slot_index(ids, experts, capacity):
    flat_ids = ids.reshape(-1)
    matches = (flat_ids[:, None] == jnp.arange(experts, dtype=jnp.int32)[None, :]).astype(jnp.int32)
    before = jnp.cumsum(matches, axis=0) - matches
    return flat_ids * capacity + jnp.sum(before * matches, axis=1)


def local(
    memory_queries,
    memory_keys,
    memory_values,
    input_gate_logits,
    forget_gate_logits,
    extra_log_decay,
    residual,
    cell_output_weight,
    expert_norm_gain,
    expert_gate_weight,
    expert_up_weight,
    expert_down_weight,
    routed_expert_index,
    routed_expert_weight,
):
    hidden, heads_here, head_dim = matrix_memory_step(
        memory_queries,
        memory_keys,
        memory_values,
        input_gate_logits,
        forget_gate_logits,
        extra_log_decay,
    )
    weight_piece = lax.all_gather(cell_output_weight, "sp", axis=1, tiled=True)
    shaped = weight_piece.reshape(heads_here, head_dim, weight_piece.shape[1])
    partial_rows = jnp.einsum(
        "htd,hdc->tc", hidden, shaped, preferred_element_type=jnp.float32
    ).astype(jnp.bfloat16)
    row_count, model_width = residual.shape
    projected = collect(partial_rows.reshape(4, 4, row_count // 4, model_width), False)
    projected = projected.reshape(row_count, model_width).astype(jnp.float32)
    mixed_rows = (residual.astype(jnp.float32) + projected).astype(jnp.bfloat16)
    mixed_wide = mixed_rows.astype(jnp.float32)
    norm_scale = lax.rsqrt(jnp.mean(mixed_wide * mixed_wide, axis=-1, keepdims=True) + epsilon)
    normed = (mixed_wide * norm_scale * expert_norm_gain).astype(jnp.bfloat16)
    sp_size = lax.axis_size("sp")
    top_count = routed_expert_index.shape[1]
    experts = sp_size * expert_gate_weight.shape[0]
    assigned = row_count * top_count
    capacity = max(2, assigned * 5 // (4 * experts))
    own_ids = lax.dynamic_slice_in_dim(
        routed_expert_index, lax.axis_index("tp") * row_count, row_count, 0
    )
    own_slots = slot_index(own_ids, experts, capacity)
    zero_row = jnp.zeros((1, model_width), jnp.bfloat16)
    padded = jnp.concatenate([normed, zero_row], axis=0)
    slot_table = jnp.full((experts * capacity,), row_count, jnp.int32)
    slot_table = slot_table.at[own_slots].set(jnp.arange(assigned, dtype=jnp.int32) // top_count)
    arrived = dispatch(padded[slot_table.reshape(experts, capacity)])
    flat_rows = arrived.reshape(-1, model_width)
    gate_pre = jnp.dot(flat_rows, expert_gate_weight[0], preferred_element_type=jnp.float32)
    up_pre = jnp.dot(flat_rows, expert_up_weight[0], preferred_element_type=jnp.float32)
    hidden_act = (jax.nn.silu(gate_pre) * up_pre).astype(jnp.bfloat16)
    group_term = jnp.dot(hidden_act, expert_down_weight[0], preferred_element_type=jnp.float32)
    group_term = lax.optimization_barrier(group_term.astype(jnp.bfloat16)).astype(jnp.float32)
    returned = collect(group_term.astype(jnp.bfloat16).reshape(arrived.shape), True)
    picked = returned.reshape(experts * capacity, model_width)[own_slots]
    picked = picked.reshape(row_count, top_count, model_width).astype(jnp.float32)
    routed_sum = jnp.sum(picked * routed_expert_weight[:, :, None], axis=1)
    return (mixed_wide + routed_sum).astype(jnp.bfloat16)


def solution(mesh):
    return jax.shard_map(
        local,
        mesh=mesh,
        in_specs=(
            P("sp", "tp"),
            P("sp", "tp"),
            P("sp", "tp"),
            P("tp", "sp"),
            P("tp", "sp"),
            P("tp", "sp"),
            P(("sp", "tp"), None),
            P("tp", "sp"),
            P(),
            P("sp", None, "tp"),
            P("sp", None, "tp"),
            P("sp", "tp", None),
            P("sp", None),
            P(("sp", "tp"), None),
        ),
        out_specs=P(("sp", "tp"), None),
        check_vma=False,
    )
```

```python
import functools
import jax
import jax.numpy as jnp
from jax import lax
from jax.experimental import pallas as pl
from jax.experimental.pallas import tpu as pltpu
from jax.sharding import PartitionSpec as P

highest = lax.Precision.HIGHEST
lowest = -1e30
epsilon = 1e-06


def places():
    sp, tp = lax.axis_index("sp"), lax.axis_index("tp")
    n = lax.axis_size("sp")
    return sp, tp, n, tp + 1 - 2 * (tp % 2), (tp + 2) % 4


def greet(devices):
    barrier = pltpu.get_barrier_semaphore()
    for device in devices:
        pl.semaphore_signal(
            barrier, inc=1, device_id=device, device_id_type=pl.DeviceIdType.MESH
        )
    pl.semaphore_wait(barrier, len(devices))


def remote(src, dst, send, recv, device):
    return pltpu.make_async_remote_copy(
        src_ref=src,
        dst_ref=dst,
        send_sem=send,
        recv_sem=recv,
        device_id=device,
        device_id_type=pl.DeviceIdType.MESH,
    )


def far_first(n):
    return sorted(range(1, n), key=lambda k: abs(2 * k - n))


def dispatch_kernel(x_ref, out_ref, send_sems, recv_sems):
    sp, tp, n, p, q = places()
    peers = [((sp + k) % n, tp) for k in range(1, n)]
    greet(peers + [(sp, p), (sp, q)])
    across, first, late = {}, {}, []
    for k in far_first(n):
        copy = remote(
            x_ref.at[(sp + k) % n], out_ref.at[tp, sp],
            send_sems.at[0, k], recv_sems.at[0, k], peers[k - 1],
        )
        copy.start()
        first[k] = copy

    def relay(k):
        across[k].wait_recv()
        s = (sp - k + n) % n
        copy = remote(
            out_ref.at[q, s], out_ref.at[q, s], send_sems.at[3, k], recv_sems.at[3, k], (sp, p)
        )
        copy.start()
        late.append(copy)

    order = [0] + far_first(n)
    for step, k in enumerate(order):
        s = (sp - k + n) % n
        if k == 0:
            src = x_ref.at[sp]
        else:
            first[k].wait_recv()
            src = out_ref.at[tp, s]
        copy = remote(src, out_ref.at[tp, s], send_sems.at[1, k], recv_sems.at[1, k], (sp, q))
        copy.start()
        across[k] = copy
        copy = remote(src, out_ref.at[tp, s], send_sems.at[2, k], recv_sems.at[2, k], (sp, p))
        copy.start()
        late.append(copy)
        if k == 0:
            out_ref[tp, sp] = x_ref[sp]
        else:
            relay(order[step - 1])
    relay(order[-1])
    for copy in late:
        copy.wait()
    for copy in list(first.values()) + list(across.values()):
        copy.wait_send()


def dispatch(x):
    n, rows, width = x.shape
    return pl.pallas_call(
        dispatch_kernel,
        out_shape=jax.ShapeDtypeStruct((4, n, rows, width), x.dtype),
        in_specs=[pl.BlockSpec(memory_space=pltpu.VMEM)],
        out_specs=pl.BlockSpec(memory_space=pltpu.VMEM),
        scratch_shapes=[pltpu.SemaphoreType.DMA((4, n)), pltpu.SemaphoreType.DMA((4, n))],
        compiler_params=pltpu.CompilerParams(
            collective_id=1, has_side_effects=True, vmem_limit_bytes=58 * 2**20
        ),
    )(x)


def collect_kernel(back, x_ref, out_ref, near, sent, far, result, send_sems, recv_sems):
    sp, tp, n, p, q = places()
    chunks = x_ref.shape[1]
    offsets = far_first(n) + [0]
    peers = [((sp + k) % n, tp) for k in offsets[:-1]] if back else []
    greet(peers + [(sp, p), (sp, q)])

    def at(k):
        return (sp + offsets[k]) % n if back else k

    near_far, near_own, crossing, homeward = [], [], [], []
    for k in range(chunks):
        copy = remote(
            x_ref.at[(p + 2) % 4, at(k)], near.at[0, k],
            send_sems.at[0, k], recv_sems.at[0, k], (sp, p),
        )
        copy.start()
        near_far.append(copy)
    for k in range(chunks):
        copy = remote(
            x_ref.at[p, at(k)], near.at[1, k], send_sems.at[1, k], recv_sems.at[1, k], (sp, p)
        )
        copy.start()
        near_own.append(copy)
    for k in range(chunks):
        near_far[k].wait_recv()
        total = x_ref[q, at(k)].astype(jnp.float32) + near[0, k].astype(jnp.float32)
        sent[k] = total.astype(jnp.bfloat16)
        copy = remote(sent.at[k], far.at[k], send_sems.at[2, k], recv_sems.at[2, k], (sp, q))
        copy.start()
        crossing.append(copy)
    for k in range(chunks):
        near_own[k].wait_recv()
        crossing[k].wait_recv()
        total = x_ref[tp, at(k)].astype(jnp.float32) + near[1, k].astype(jnp.float32)
        total = (total + far[k].astype(jnp.float32)).astype(jnp.bfloat16)
        if not back:
            out_ref[k] = total
        elif k == chunks - 1:
            out_ref[sp] = total
        else:
            result[k] = total
            copy = remote(
                result.at[k], out_ref.at[sp], send_sems.at[3, k], recv_sems.at[3, k], peers[k]
            )
            copy.start()
            homeward.append(copy)
    for copy in homeward:
        copy.wait()
    for copy in near_far + near_own + crossing:
        copy.wait_send()


def collect(x, back):
    _, n, rows, width = x.shape
    block = (n, rows, width)
    return pl.pallas_call(
        functools.partial(collect_kernel, back),
        out_shape=jax.ShapeDtypeStruct(block, x.dtype),
        in_specs=[pl.BlockSpec(memory_space=pltpu.VMEM)],
        out_specs=pl.BlockSpec(memory_space=pltpu.VMEM),
        scratch_shapes=[
            pltpu.VMEM((2,) + block, x.dtype),
            pltpu.VMEM(block, x.dtype),
            pltpu.VMEM(block, x.dtype),
            pltpu.VMEM(block if back else (1, 16, 128), x.dtype),
            pltpu.SemaphoreType.DMA((4, n)),
            pltpu.SemaphoreType.DMA((4, n)),
        ],
        compiler_params=pltpu.CompilerParams(
            collective_id=2 if back else 3, has_side_effects=True, vmem_limit_bytes=58 * 2**20
        ),
    )(x)


def spread_kernel(x_ref, out_ref, send_sems, recv_sems):
    sp, tp, n, _, _ = places()
    half = n // 2
    twin = sp + 1 - 2 * (sp % 2)
    peers = [((sp + 2 * k) % n, tp) for k in range(1, half)]
    greet(peers + [(twin, tp)])
    first, second = [None], []
    for k in range(1, half):
        copy = remote(
            x_ref, out_ref.at[sp], send_sems.at[0, k], recv_sems.at[0, k], peers[k - 1]
        )
        copy.start()
        first.append(copy)
    for k in range(half):
        s = (sp - 2 * k + n) % n
        if k == 0:
            src = x_ref
        else:
            first[k].wait_recv()
            src = out_ref.at[s]
        copy = remote(src, out_ref.at[s], send_sems.at[1, k], recv_sems.at[1, k], (twin, tp))
        copy.start()
        second.append(copy)
        if k == 0:
            out_ref[sp] = x_ref[...]
    for copy in second:
        copy.wait()
    for copy in first[1:]:
        copy.wait_send()


def spread(x):
    n = lax.axis_size("sp")
    half = n // 2
    return pl.pallas_call(
        spread_kernel,
        out_shape=jax.ShapeDtypeStruct((n,) + x.shape, x.dtype),
        in_specs=[pl.BlockSpec(memory_space=pltpu.VMEM)],
        out_specs=pl.BlockSpec(memory_space=pltpu.VMEM),
        scratch_shapes=[pltpu.SemaphoreType.DMA((2, half)), pltpu.SemaphoreType.DMA((2, half))],
        compiler_params=pltpu.CompilerParams(
            collective_id=4, has_side_effects=True, vmem_limit_bytes=58 * 2**20
        ),
    )(x)


def carried_in(x):
    log_sum, mat, norm, top = x
    heads, dim, _ = mat.shape
    n, place = lax.axis_size("sp"), lax.axis_index("sp")
    scalars = jnp.broadcast_to(jnp.concatenate([log_sum, top])[:, None], (2 * heads, dim))
    packed = jnp.concatenate([mat.reshape(heads * dim, dim), norm, scalars], axis=0)
    used = packed.shape[0]
    packed = jnp.pad(packed, ((0, -used % 8), (0, 0)))
    everything = spread(packed)
    mats = everything[:, : heads * dim].reshape(n, heads, dim, dim)
    norms = everything[:, heads * dim : heads * dim + heads]
    logs = everything[:, heads * dim + heads : heads * dim + 2 * heads, 0]
    tops = everything[:, heads * dim + 2 * heads : heads * dim + 3 * heads, 0]
    index = jnp.arange(n)
    reached = index < place
    between = (index[None, :] > index[:, None]) & reached[None, :]
    decay = jnp.sum(jnp.where(between[:, :, None], logs[None], 0.0), axis=1)
    level = jnp.where(reached[:, None], tops + decay, lowest)
    prior_max = jnp.max(level, axis=0)
    scale = jnp.where(reached[:, None], jnp.exp(level - prior_max), 0.0)
    prior_mat = jnp.sum(scale[:, :, None, None] * mats, axis=0)
    prior_norm = jnp.sum(scale[:, :, None] * norms, axis=0)
    return prior_mat, prior_norm, prior_max


def block_pass(memory, inputs):
    state_mat, state_norm, state_max = memory
    queries, keys_blk, values_blk, gate_in, forget_log_value = inputs
    length = gate_in.shape[-1]
    running = jnp.cumsum(forget_log_value, axis=-1)
    causal = jnp.arange(length)[:, None] >= jnp.arange(length)[None, :]
    exponent = running[:, :, None] - running[:, None, :] + gate_in[:, None, :]
    exponent = jnp.where(causal[None], exponent, -jnp.inf)
    carried = running + state_max[:, None]
    row_max = jnp.maximum(carried, jnp.max(exponent, axis=-1))
    decays = jnp.exp(exponent - row_max[:, :, None])
    carry_scale = jnp.exp(carried - row_max)
    dispatch_affinity = jnp.einsum("htk,hsk->hts", queries, keys_blk, precision=highest) * decays
    numerator = carry_scale[:, :, None] * jnp.einsum(
        "hvk,htk->htv", state_mat, queries, precision=highest
    )
    numerator = numerator + jnp.einsum(
        "hts,hsv->htv", dispatch_affinity, values_blk, precision=highest
    )
    denominator = carry_scale * jnp.einsum(
        "hk,htk->ht", state_norm, queries, precision=highest
    ) + jnp.sum(dispatch_affinity, axis=-1)
    final_log = running[:, -1]
    log_prev = final_log + state_max
    log_keep = final_log[:, None] - running + gate_in
    new_max = jnp.maximum(log_prev, jnp.max(log_keep, axis=-1))
    prev_scale = jnp.exp(log_prev - new_max)
    retain = jnp.exp(log_keep - new_max[:, None])
    new_mat = prev_scale[:, None, None] * state_mat + jnp.einsum(
        "hsv,hsk->hvk", retain[:, :, None] * values_blk, keys_blk, precision=highest
    )
    new_norm = prev_scale[:, None] * state_norm + jnp.einsum(
        "hs,hsk->hk", retain, keys_blk, precision=highest
    )
    return ((new_mat, new_norm, new_max), (numerator, denominator, row_max))


def matrix_memory_step(
    memory_queries,
    memory_keys,
    memory_values,
    input_gate_logits,
    forget_gate_logits,
    extra_log_decay,
):
    tokens_here, channels = memory_queries.shape
    heads_here = input_gate_logits.shape[0]
    head_dim = channels // heads_here

    def heads_first(tensor):
        pieces = [
            tensor[:, head * head_dim : (head + 1) * head_dim] for head in range(heads_here)
        ]
        return jnp.stack(pieces).astype(jnp.float32)

    queries = heads_first(memory_queries) * head_dim ** (-0.5)
    forget_log_value = jax.nn.log_sigmoid(forget_gate_logits) + extra_log_decay
    block_size = min(tokens_here, 256)
    block_count = tokens_here // block_size

    def split_blocks(tensor):
        return jnp.moveaxis(
            tensor.reshape((heads_here, block_count, block_size) + tensor.shape[2:]), 1, 0
        )

    def join_blocks(tensor):
        return jnp.moveaxis(tensor, 0, 1).reshape((heads_here, tokens_here) + tensor.shape[3:])

    empty_state = (
        jnp.zeros((heads_here, head_dim, head_dim), jnp.float32),
        jnp.zeros((heads_here, head_dim), jnp.float32),
        jnp.full((heads_here,), lowest, jnp.float32),
    )
    members = (
        queries,
        heads_first(memory_keys),
        heads_first(memory_values),
        input_gate_logits,
        forget_log_value,
    )
    end_state, pieces = lax.scan(
        block_pass, empty_state, tuple((split_blocks(member) for member in members))
    )
    numerator, denominator, row_max = (join_blocks(member) for member in pieces)
    running = jnp.cumsum(forget_log_value, axis=-1)
    prior_mat, prior_norm, prior_max = carried_in((running[:, -1],) + tuple(end_state))
    reached = running + prior_max[:, None]
    joined = jnp.maximum(row_max, reached)
    local_scale = jnp.exp(row_max - joined)
    carry_scale = jnp.exp(reached - joined)
    numerator = local_scale[:, :, None] * numerator + carry_scale[:, :, None] * jnp.einsum(
        "hvk,htk->htv", prior_mat, queries, precision=highest
    )
    denominator = local_scale * denominator + carry_scale * jnp.einsum(
        "hk,htk->ht", prior_norm, queries, precision=highest
    )
    guarded = jnp.maximum(jnp.abs(denominator), jnp.exp(-joined))
    return ((numerator / guarded[:, :, None]).astype(jnp.bfloat16), heads_here, head_dim)


def slot_index(ids, experts, capacity):
    flat_ids = ids.reshape(-1)
    matches = (flat_ids[:, None] == jnp.arange(experts, dtype=jnp.int32)[None, :]).astype(jnp.int32)
    before = jnp.cumsum(matches, axis=0) - matches
    return flat_ids * capacity + jnp.sum(before * matches, axis=1)


def local(
    memory_queries,
    memory_keys,
    memory_values,
    input_gate_logits,
    forget_gate_logits,
    extra_log_decay,
    residual,
    cell_output_weight,
    expert_norm_gain,
    expert_gate_weight,
    expert_up_weight,
    expert_down_weight,
    routed_expert_index,
    routed_expert_weight,
):
    hidden, heads_here, head_dim = matrix_memory_step(
        memory_queries,
        memory_keys,
        memory_values,
        input_gate_logits,
        forget_gate_logits,
        extra_log_decay,
    )
    weight_piece = lax.all_gather(cell_output_weight, "sp", axis=1, tiled=True)
    shaped = weight_piece.reshape(heads_here, head_dim, weight_piece.shape[1])
    partial_rows = jnp.einsum(
        "htd,hdc->tc", hidden, shaped, preferred_element_type=jnp.float32
    ).astype(jnp.bfloat16)
    row_count, model_width = residual.shape
    projected = collect(partial_rows.reshape(4, 4, row_count // 4, model_width), False)
    projected = projected.reshape(row_count, model_width).astype(jnp.float32)
    mixed_rows = (residual.astype(jnp.float32) + projected).astype(jnp.bfloat16)
    mixed_wide = mixed_rows.astype(jnp.float32)
    norm_scale = lax.rsqrt(jnp.mean(mixed_wide * mixed_wide, axis=-1, keepdims=True) + epsilon)
    normed = (mixed_wide * norm_scale * expert_norm_gain).astype(jnp.bfloat16)
    sp_size = lax.axis_size("sp")
    top_count = routed_expert_index.shape[1]
    experts = sp_size * expert_gate_weight.shape[0]
    assigned = row_count * top_count
    capacity = max(2, assigned * 5 // (4 * experts))
    own_ids = lax.dynamic_slice_in_dim(
        routed_expert_index, lax.axis_index("tp") * row_count, row_count, 0
    )
    own_slots = slot_index(own_ids, experts, capacity)
    slots = own_slots.reshape(row_count, top_count)
    at_slot = slots[:, :, None] == jnp.arange(experts * capacity, dtype=jnp.int32)
    chosen = jnp.any(at_slot, axis=1).astype(jnp.bfloat16)
    outgoing = lax.dot_general(
        chosen, normed, (((0,), (0,)), ((), ())), preferred_element_type=jnp.float32
    ).astype(jnp.bfloat16)
    arrived = dispatch(outgoing.reshape(experts, capacity, model_width))
    flat_rows = arrived.reshape(-1, model_width)
    gate_pre = jnp.dot(flat_rows, expert_gate_weight[0], preferred_element_type=jnp.float32)
    up_pre = jnp.dot(flat_rows, expert_up_weight[0], preferred_element_type=jnp.float32)
    hidden_act = (jax.nn.silu(gate_pre) * up_pre).astype(jnp.bfloat16)
    group_term = jnp.dot(hidden_act, expert_down_weight[0], preferred_element_type=jnp.float32)
    group_term = lax.optimization_barrier(group_term.astype(jnp.bfloat16)).astype(jnp.float32)
    returned = collect(group_term.astype(jnp.bfloat16).reshape(arrived.shape), True)
    share = jnp.sum(jnp.where(at_slot, routed_expert_weight[:, :, None], 0.0), axis=1)
    routed_sum = jnp.dot(
        share,
        returned.reshape(experts * capacity, model_width).astype(jnp.float32),
        precision=highest,
    )
    return (mixed_wide + routed_sum).astype(jnp.bfloat16)


def solution(mesh):
    return jax.shard_map(
        local,
        mesh=mesh,
        in_specs=(
            P("sp", "tp"),
            P("sp", "tp"),
            P("sp", "tp"),
            P("tp", "sp"),
            P("tp", "sp"),
            P("tp", "sp"),
            P(("sp", "tp"), None),
            P("tp", "sp"),
            P(),
            P("sp", None, "tp"),
            P("sp", None, "tp"),
            P("sp", "tp", None),
            P("sp", None),
            P(("sp", "tp"), None),
        ),
        out_specs=P(("sp", "tp"), None),
        check_vma=False,
    )
```
